32 devices in a mesh: ep: 8 (over z, core), tp: 4 (over y, x).
Axes of the slice: x: 2, y: 2, z: 4, core: 2. Of those that a mesh axis runs over, the one named last changes fastest.
Arguments:
- tokens: bfloat16 [128, 1024], P('ep'), may hold values from -6 to 6
- kv_cache: bfloat16 [128, 1024, 16, 128], P('ep', None, 'tp'), may hold values from -6 to 6
- lengths: int32 [128], P('ep'), may hold values from 1 to 1024, 65536 in all
- score_offset: float32 [16], P('tp'), may hold values from 3 to 9
- mixer_gain: float32 [1024], replicated, may hold values from 0.1 to 1.9
- query_weight: bfloat16 [1024, 1024], P(None, 'tp'), may hold values from -0.1875 to 0.1875
- key_weight: bfloat16 [1024, 1024], P(None, 'tp'), may hold values from -0.1875 to 0.1875
- value_weight: bfloat16 [1024, 1024], P(None, 'tp'), may hold values from -0.1875 to 0.1875
- out_weight: bfloat16 [1024, 1024], P('tp'), may hold values from -0.75 to 0.75
- channel_gain: float32 [1024], replicated, may hold values from 0.1 to 1.9
- routes: int32 [128, 2], P('ep'), may hold values from 0 to 7, all different within a row; in each aligned block of 16 rows (0 to 15, 16 to 31, ...) at most 8 rows name the same one
- route_weights: float32 [128, 2], P('ep'), may hold values from 0.25 to 1
- gate_weight: bfloat16 [8, 1024, 2048], P('ep', None, 'tp'), may hold values from -0.1875 to 0.1875
- up_weight: bfloat16 [8, 1024, 2048], P('ep', None, 'tp'), may hold values from -0.1875 to 0.1875
- down_weight: bfloat16 [8, 2048, 1024], P('ep', 'tp'), may hold values from -0.125 to 0.125
Outputs:
- mixed: bfloat16 [128, 1024], P('ep', 'tp')
- new_entries: bfloat16 [128, 16, 128], P('ep', 'tp')
The draws below stay inside these ranges and needn't reach their ends.
Inputs may be any that keep to these rules, and one draw needn't show every extreme that they name: `routes`: each row names 2 different experts; within the rows of one index of ep (aligned blocks of 16 rows) no expert is named more than 8 times. `lengths`: some sequence fills all 1024 positions.
All inputs are finite; a program needn't handle non-finite values. No bound on the sum of `lengths` on one device may be relied on, other than what follows from the above.
Results may differ from the reference program's by a relative error of at most 0.017.
Values may be sent and summed in bfloat16 or wider, within the bound.
A program may use at most 128 MiB of HBM per device.

```python
import math
import jax
import jax.numpy as jnp
import numpy as np
from jax import lax

D = 1024
HEADS = 16
HEAD_DIM = 64
FF = 2048
TOP_K = 2
SEQ_DEV = 16
CACHE = 1024
SEQS = 128
EXPERTS = 8
CAP = 8
N_TP = 4


def draw_kv_cache(key, part):
    base = jax.random.fold_in(key, 23)
    mean_key, sign_key, noise_key = jax.random.split(base, 3)
    shape = (SEQS, CACHE, HEADS, 2 * HEAD_DIM)
    channel_sign = jnp.where(jax.random.bernoulli(sign_key, 0.5, (HEADS, 2 * HEAD_DIM)), 1.0, -1.0)
    value_mean = channel_sign * jax.random.uniform(mean_key, (HEADS, 2 * HEAD_DIM), jnp.float32, 0.5, 1.5)
    noise = jax.random.normal(noise_key, shape, jnp.float32)
    value_part = jnp.arange(2 * HEAD_DIM, dtype=jnp.int32) >= HEAD_DIM
    shift = jnp.where(value_part[None, :], value_mean, 0.0)
    return jnp.clip(noise + shift[None, None, :, :], -6.0, 6.0).astype(jnp.bfloat16)


def draw_score_offset(key, part):
    base = jax.random.fold_in(key, 11)
    pick_key, slow_key, fast_key = jax.random.split(base, 3)
    fast_value = jax.random.uniform(fast_key, (HEADS,), jnp.float32, 3.0, 4.0)
    slow_heads = jax.random.uniform(pick_key, (HEADS,), jnp.float32) < 0.5
    slow_value = jax.random.uniform(slow_key, (HEADS,), jnp.float32, 6.5, 9.0)
    return jnp.where(slow_heads, slow_value, fast_value).astype(jnp.float32)


def block_scale(own_key, shape, shards, low, top_value):
    gain, own = 1.0, jax.random.fold_in(own_key, 6)
    for dim, shards_of in shards:
        draws = jnp.exp(jax.random.uniform(jax.random.fold_in(own, dim), (shards_of,), jnp.float32, low / len(shards), top_value / len(shards)))
        gain = gain * jnp.repeat(draws, shape[dim] // shards_of).reshape([-1 if axis == dim else 1 for axis in range(len(shape))])
    return gain


def length_profile(count, total, bound, skew):
    weights = [(1 << 20) // math.isqrt(standing ** skew) + 1 for standing in range(2, count + 1)]
    rest, counts = total - bound - (count - 1), [1] * (count - 1)
    while rest > 0:
        free = [i for i in range(count - 1) if counts[i] < bound]
        pool, remaining = sum([weights[i] for i in free]), rest
        for i in free:
            more = min(bound - counts[i], max(1, remaining * weights[i] // pool), rest)
            counts[i] = counts[i] + more
            rest = rest - more
    return np.array([bound] + counts)


def ragged_sizes(key, count, total, bound, slope):
    if count == 2:
        one = jax.random.randint(key, (), max(1, total - bound), min(bound, total - 1) + 1)
        return jnp.stack([one, total - one])
    sizes = jnp.asarray(length_profile(count, total, bound, slope), jnp.int32)
    couples = (count - 1) // 2
    donor, taker = sizes[1:1 + 2 * couples:2], sizes[2:2 + 2 * couples:2]
    room = jnp.minimum(donor - 1, bound - taker)
    passed = jax.random.randint(jax.random.fold_in(key, 1), (couples,), 0, 1 << 20) % (room + 1)
    sizes = sizes.at[1:1 + 2 * couples:2].set(donor - passed).at[2:2 + 2 * couples:2].set(taker + passed)
    return sizes[jax.random.permutation(jax.random.fold_in(key, 2), count)]


def deal_out(key, own, number, rows, count, top, most, skew):
    order = jax.random.permutation(key, count)
    heavy_load, common = shares(count, rows * top, most, skew, True), shares(count, rows * top, most, skew, False)
    places = jnp.arange(count)

    def named(sizes, offset_by):
        used = int((sizes > 0).sum())
        fixed = max(1, used // 4)
        moved = fixed + (places - fixed + offset_by * (used - fixed)) % max(1, count - fixed)
        return jnp.zeros((count,), jnp.int32).at[order[jnp.where(places < fixed, places, moved)]].set(jnp.asarray(sizes, jnp.int32))

    sizes = jnp.where(number % 4 == 0, named(heavy_load, number // 4), named(common, number - number // 4 - 1))
    mixed = jax.random.permutation(jax.random.fold_in(own, 3), count)
    giver, taker = mixed[0:count // 2 * 2:2], mixed[1:count // 2 * 2:2]
    margin = jnp.minimum(sizes[giver] - 1, most - sizes[taker]) // 2
    margin = jnp.where((giver == order[0]) | (taker == order[0]) | (sizes[taker] == 0), 0, jnp.maximum(margin, 0))
    moved = jax.random.randint(jax.random.fold_in(own, 4), (count // 2,), 0, 1 << 20) % (margin + 1)
    sizes = sizes.at[giver].add(-moved).at[taker].add(moved)
    items = jnp.searchsorted(jnp.cumsum(sizes), jnp.arange(rows * top), side="right").astype(jnp.int32)
    grid = items.reshape(top, rows).T
    grid = grid[jax.random.permutation(jax.random.fold_in(own, 1), rows)]
    offset_by = jax.random.randint(jax.random.fold_in(own, 2), (rows, 1), 0, top)
    return jnp.take_along_axis(grid, (jnp.arange(top)[None, :] + offset_by) % top, axis=1)


def shares(amount, total, reach, skew, full):
    loads = [(1 << 20) // math.isqrt(grade ** skew) + 1 for grade in range(1, amount + 1)]
    largest = reach if full else min(reach, max(-(-total // amount), total * loads[0] // sum(loads)))
    least = 1 if total - largest >= amount - 1 else 0
    counts, spare = [largest] + [least] * (amount - 1), total - largest - least * (amount - 1)
    while spare > 0:
        movable = [i for i in range(1, amount) if counts[i] < largest] or [i for i in range(1, amount) if counts[i] < reach]
        pool, left = sum([loads[i] for i in movable]), spare
        for i in movable:
            more = min(reach - counts[i], max(1, left * loads[i] // pool), spare)
            counts[i] = counts[i] + more
            spare = spare - more
    return np.array(counts)


def scatter_about(stream_key, dims, spread, bound, shards=(), kind=jnp.bfloat16):
    values = spread * jax.random.normal(stream_key, dims, jnp.float32)
    if shards:
        values = values * block_scale(stream_key, dims, shards, -0.22, 0.18)
    return jnp.clip(values, -bound, bound).astype(kind)


def setup_inputs(seed: int = 0) -> dict:
    key_of = jax.random.split(jax.random.key(seed), 16)
    tokens = scatter_about(key_of[0], (SEQS, D), 1.0, 6.0, ((0, 8),))
    kv_cache = draw_kv_cache(jax.random.fold_in(key_of[15], 71), 0)
    lengths = ragged_sizes(key_of[2], SEQS, SEQS * CACHE // 2, CACHE, 2).astype(jnp.int32)
    score_offset = draw_score_offset(jax.random.fold_in(key_of[15], 71), 0)
    mixer_gain = jnp.clip(1.0 + 0.18 * jax.random.normal(key_of[4], (D,), jnp.float32), 0.1, 1.9)
    query_weight = scatter_about(key_of[5], (D, HEADS * HEAD_DIM), D ** -0.5, 0.1875, ((1, 4),))
    key_weight = scatter_about(key_of[6], (D, HEADS * HEAD_DIM), D ** -0.5, 0.1875, ((1, 4),))
    value_weight = scatter_about(key_of[7], (D, HEADS * HEAD_DIM), D ** -0.5, 0.1875, ((1, 4),))
    out_weight = scatter_about(key_of[8], (HEADS * HEAD_DIM, D), (HEADS * HEAD_DIM // 16) ** -0.5, 0.75, ((0, 4),))
    channel_gain = jnp.clip(1.0 + 0.18 * jax.random.normal(key_of[9], (D,), jnp.float32), 0.1, 1.9)
    routes_keys = jax.random.split(jax.random.fold_in(key_of[10], 1), SEQS // SEQ_DEV)
    routes_turns = jax.random.permutation(jax.random.fold_in(key_of[10], 3), SEQS // SEQ_DEV)
    routes = jax.vmap(lambda own, number: deal_out(jax.random.fold_in(key_of[10], 2), own, number, SEQ_DEV, EXPERTS, TOP_K, CAP, 2))(routes_keys, routes_turns).reshape((SEQS, TOP_K))
    route_weights = jnp.clip(0.25 + 0.75 * jax.random.uniform(key_of[11], (SEQS, TOP_K), jnp.float32) ** block_scale(key_of[11], (SEQS, TOP_K), ((0, 8),), -0.2, 0.2), 0.25, 1.0)
    gate_weight = scatter_about(key_of[12], (EXPERTS, D, FF), D ** -0.5, 0.1875, ((0, 8), (2, 4)))
    up_weight = scatter_about(key_of[13], (EXPERTS, D, FF), D ** -0.5, 0.1875, ((0, 8), (2, 4)))
    down_weight = scatter_about(key_of[14], (EXPERTS, FF, D), FF ** -0.5, 0.125, ((0, 8), (1, 4)))
    return {"tokens": tokens, "kv_cache": kv_cache, "lengths": lengths, "score_offset": score_offset, "mixer_gain": mixer_gain, "query_weight": query_weight, "key_weight": key_weight, "value_weight": value_weight, "out_weight": out_weight, "channel_gain": channel_gain, "routes": routes, "route_weights": route_weights, "gate_weight": gate_weight, "up_weight": up_weight, "down_weight": down_weight}


EPSILON = 1e-06

def rms_scale(values, scale_gain):
    return values * lax.rsqrt(lax.optimization_barrier(jnp.mean(values * values, axis=-1, keepdims=True)) + EPSILON) * scale_gain

def reference(tokens, kv_cache, lengths, score_offset, mixer_gain, query_weight, key_weight, value_weight, out_weight, channel_gain, routes, route_weights, gate_weight, up_weight, down_weight):
    seq_total = tokens.shape[0]
    head_span = HEADS * HEAD_DIM
    inputs = tokens.astype(jnp.float32)
    normed = rms_scale(inputs, mixer_gain).astype(jnp.bfloat16)
    query_rows = jnp.dot(normed, query_weight, preferred_element_type=jnp.float32).astype(jnp.bfloat16)
    key_rows = jnp.dot(normed, key_weight, preferred_element_type=jnp.float32).astype(jnp.bfloat16)
    value_rows = jnp.dot(normed, value_weight, preferred_element_type=jnp.float32).astype(jnp.bfloat16)
    new_entries = jnp.concatenate([key_rows.reshape(seq_total, HEADS, HEAD_DIM), value_rows.reshape(seq_total, HEADS, HEAD_DIM)], axis=2)
    block_count = seq_total // SEQ_DEV
    query_blocks = query_rows.reshape(block_count, SEQ_DEV, HEADS, HEAD_DIM)
    cache_blocks = kv_cache.reshape(block_count, SEQ_DEV, CACHE, HEADS, 2 * HEAD_DIM)
    length_blocks = lengths.reshape(block_count, SEQ_DEV)

    def attend(block):
        query_block, cache_block, length_block = block
        cached_keys = cache_block[..., :HEAD_DIM].astype(jnp.float32)
        cached_values = cache_block[..., HEAD_DIM:].astype(jnp.float32)
        scores = jnp.einsum('shd,sphd->shp', query_block.astype(jnp.float32), cached_keys) * HEAD_DIM ** (-0.5) - score_offset[None, :, None]
        positions = jnp.arange(CACHE, dtype=jnp.int32)
        visible = (positions[None, :] < length_block[:, None])[:, None, :]
        log_keep = jnp.where(visible, jax.nn.log_sigmoid(-scores), 0.0)
        after_sum = lax.cumsum(log_keep, axis=2, reverse=True) - log_keep
        stick_weights = jnp.where(visible, jnp.exp(jax.nn.log_sigmoid(scores) + after_sum), 0.0).astype(jnp.bfloat16)
        return jnp.einsum('shp,sphd->shd', stick_weights.astype(jnp.float32), cached_values).astype(jnp.bfloat16)
    attended = lax.map(attend, (query_blocks, cache_blocks, length_blocks)).reshape(seq_total, N_TP, head_span // N_TP)
    out_groups = out_weight.reshape(N_TP, head_span // N_TP, D)
    head_terms = jnp.einsum('sgc,gcd->sgd', attended.astype(jnp.float32), out_groups.astype(jnp.float32)).astype(jnp.bfloat16)
    residual = inputs + lax.optimization_barrier(jnp.sum(head_terms.astype(jnp.float32), axis=1))
    hidden = rms_scale(residual, channel_gain).astype(jnp.bfloat16)
    pair_rows = jnp.repeat(hidden, TOP_K, axis=0)
    pair_experts = routes.reshape(-1).astype(jnp.int32)

    def expert_one(item):
        row_vector, expert_id = item
        gate_matrix = lax.dynamic_index_in_dim(gate_weight, expert_id, 0, keepdims=False)
        up_matrix = lax.dynamic_index_in_dim(up_weight, expert_id, 0, keepdims=False)
        down_matrix = lax.dynamic_index_in_dim(down_weight, expert_id, 0, keepdims=False)
        gate_rows = jnp.dot(row_vector[None, :], gate_matrix, preferred_element_type=jnp.float32)
        upward = jnp.dot(row_vector[None, :], up_matrix, preferred_element_type=jnp.float32)
        active = (jax.nn.silu(gate_rows) * upward).astype(jnp.bfloat16)
        group_terms = jnp.einsum('gf,gfd->gd', active.reshape(N_TP, FF // N_TP).astype(jnp.float32), down_matrix.reshape(N_TP, FF // N_TP, D).astype(jnp.float32))
        rounded = lax.optimization_barrier(group_terms.astype(jnp.bfloat16))
        return lax.optimization_barrier(jnp.sum(rounded.astype(jnp.float32), axis=0)).astype(jnp.bfloat16)
    expert_out = lax.map(expert_one, (pair_rows, pair_experts)).reshape(seq_total, TOP_K, D)
    expert_mix = lax.optimization_barrier(jnp.sum(route_weights[:, :, None] * expert_out.astype(jnp.float32), axis=1))
    mixed = (residual + expert_mix).astype(jnp.bfloat16)
    return (mixed, new_entries)
```

```python
import jax
import jax.numpy as jnp
from jax import lax
from jax.experimental import pallas as pl
from jax.experimental.pallas import tpu as pltpu
from jax.sharding import PartitionSpec as P

EPSILON = 1e-06


def rms_scale(values, scale_gain):
    return (
        values * lax.rsqrt(jnp.mean(values * values, axis=-1, keepdims=True) + EPSILON) * scale_gain
    )


def attend_kernel(
    lengths_ref,
    tokens_ref,
    gain_ref,
    offset_ref,
    length_rows_ref,
    query_hbm,
    key_hbm,
    value_hbm,
    out_hbm,
    cache_hbm,
    partial_ref,
    entries_ref,
    cache_buf,
    weight_buf,
    out_buf,
    query_scr,
    score_scr,
    sum_scr,
    entry_scr,
    weight_sem,
    cache_sem,
):
    seqs, rows_all, lanes = cache_buf.shape
    heads = entries_ref.shape[1]
    head_dim = lanes // 2
    parts = cache_sem.shape[1]
    part_rows = rows_all // parts
    part_span = part_rows // heads
    blocks = rows_all // lanes
    block_span = lanes // heads

    def weight_copy(source, target, index):
        return pltpu.make_async_copy(source, target, weight_sem.at[index])

    copies = [
        weight_copy(query_hbm, weight_buf.at[0], 0),
        weight_copy(key_hbm, weight_buf.at[1], 1),
        weight_copy(value_hbm, weight_buf.at[2], 2),
        weight_copy(out_hbm, out_buf, 3),
    ]
    copies[0].start()

    def cache_copy(seq, part):
        span = pl.ds(part * part_rows, part_rows)
        return pltpu.make_async_copy(
            cache_hbm.at[seq, span], cache_buf.at[seq, span], cache_sem.at[seq, part]
        )

    def start_seq(seq, carry):
        for part in range(parts):

            @pl.when(lengths_ref[seq] > part * part_span)
            def _():
                cache_copy(seq, part).start()

        return carry

    lax.fori_loop(0, 2, start_seq, 0)
    copies[1].start()
    copies[2].start()
    lax.fori_loop(2, seqs, start_seq, 0)
    copies[3].start()

    inputs = tokens_ref[...].astype(jnp.float32)
    normed = rms_scale(inputs, gain_ref[...]).astype(jnp.bfloat16)
    query_scr[...] = jnp.zeros_like(query_scr)
    sum_scr[...] = jnp.zeros_like(sum_scr)
    copies[0].wait()
    query = jnp.dot(normed, weight_buf[0], preferred_element_type=jnp.float32)
    for head in range(heads):
        query_scr[:, head, :head_dim] = query[:, head * head_dim : (head + 1) * head_dim]

    group = query_scr.shape[1]
    row_id = lax.broadcasted_iota(jnp.int32, (group, part_rows), 0)
    lane_id = lax.broadcasted_iota(jnp.int32, (group, part_rows), 1)
    own_head = row_id == lane_id % heads

    def score_seq(seq, carry):
        query_rows = query_scr[seq].astype(jnp.bfloat16)
        for part in range(parts):

            @pl.when(lengths_ref[seq] > part * part_span)
            def _():
                cache_copy(seq, part).wait()
                rows = cache_buf[seq, part * part_rows : (part + 1) * part_rows, :]
                every = lax.dot_general(
                    query_rows, rows, (((1,), (1,)), ((), ())), preferred_element_type=jnp.float32
                )
                score_scr[pl.ds(seq, 1), part * part_rows : (part + 1) * part_rows] = jnp.sum(
                    jnp.where(own_head, every, 0.0), axis=0, keepdims=True
                )

        return carry

    lax.fori_loop(0, seqs, score_seq, 0)

    length_rows = length_rows_ref[...]
    offsets = offset_ref[...]
    lane = lax.broadcasted_iota(jnp.int32, (seqs, lanes), 1) // heads
    scores, keeps = [], []
    for block in range(blocks):
        visible = lane + block * block_span < length_rows
        score = score_scr[:, block * lanes : (block + 1) * lanes] * head_dim ** (-0.5) - offsets
        score = jnp.where(visible, score, 0.0)
        keep = -(jnp.maximum(score, 0.0) + jnp.log(1.0 + jnp.exp(-jnp.abs(score))))
        keep = jnp.where(visible, keep, 0.0)
        score_scr[:, block * lanes : (block + 1) * lanes] = score + keep
        keeps.append(keep)
    keep_all = jnp.concatenate(keeps, axis=0)
    keep_high = keep_all.astype(jnp.bfloat16)
    keep_low = (keep_all - keep_high.astype(jnp.float32)).astype(jnp.bfloat16)
    from_id = lax.broadcasted_iota(jnp.int32, (2 * lanes, 2 * lanes), 0) % lanes
    to_id = lax.broadcasted_iota(jnp.int32, (2 * lanes, 2 * lanes), 1)
    same = from_id % heads == to_id % heads
    later = (to_id >= lanes) | (from_id // heads > (to_id % lanes) // heads)
    summing = jnp.where(same & later, 1.0, 0.0).astype(jnp.bfloat16)
    summed = jnp.dot(
        jnp.concatenate([keep_high, keep_low], axis=1), summing, preferred_element_type=jnp.float32
    )
    carry = jnp.zeros((seqs, lanes), jnp.float32)
    for block in reversed(range(blocks)):
        visible = lane + block * block_span < length_rows
        piece = summed[block * seqs : (block + 1) * seqs]
        exponent = score_scr[:, block * lanes : (block + 1) * lanes] + piece[:, :lanes] + carry
        score_scr[:, block * lanes : (block + 1) * lanes] = jnp.where(
            visible, jnp.exp(exponent), 0.0
        )
        carry = carry + piece[:, lanes:]

    def value_seq(seq, carry):
        for part in range(parts):

            @pl.when(lengths_ref[seq] > part * part_span)
            def _():
                rows = cache_buf[seq, part * part_rows : (part + 1) * part_rows, :]
                sticks = score_scr[pl.ds(seq, 1), part * part_rows : (part + 1) * part_rows]
                sticks = jnp.where(
                    own_head, jnp.broadcast_to(sticks, own_head.shape), 0.0
                ).astype(jnp.bfloat16)
                sum_scr[seq] += jnp.dot(sticks, rows, preferred_element_type=jnp.float32)

        return carry

    lax.fori_loop(0, seqs, value_seq, 0)

    copies[1].wait()
    copies[2].wait()
    key = jnp.dot(normed, weight_buf[1], preferred_element_type=jnp.float32)
    value = jnp.dot(normed, weight_buf[2], preferred_element_type=jnp.float32)
    for head in range(heads):
        span = slice(head * head_dim, (head + 1) * head_dim)
        entry_scr[:, head, :] = jnp.concatenate([key[:, span], value[:, span]], axis=1)
    entries_ref[...] = entry_scr[...].astype(entries_ref.dtype)

    attended = jnp.concatenate(
        [sum_scr[:, head, head_dim:] for head in range(heads)], axis=1
    ).astype(jnp.bfloat16)
    copies[3].wait()
    partial_ref[...] = jnp.dot(
        attended, out_buf[...], preferred_element_type=jnp.float32
    ).astype(partial_ref.dtype)


def attend(
    tokens, kv_cache, lengths, score_offset, mixer_gain, query_weight, key_weight, value_weight, out_weight
):
    seqs, span, heads, lanes = kv_cache.shape
    width = tokens.shape[1]
    columns = query_weight.shape[1]
    parts = 4 if span % 4 == 0 and (span // 4 * heads) % lanes == 0 else 1
    vmem = pl.BlockSpec(memory_space=pltpu.VMEM)
    hbm = pl.BlockSpec(memory_space=pl.ANY)
    return pl.pallas_call(
        attend_kernel,
        name="attend",
        out_shape=(
            jax.ShapeDtypeStruct((seqs, width), jnp.bfloat16),
            jax.ShapeDtypeStruct((seqs, heads, lanes), jnp.bfloat16),
        ),
        in_specs=[pl.BlockSpec(memory_space=pltpu.SMEM)] + [vmem] * 4 + [hbm] * 5,
        out_specs=(vmem, vmem),
        scratch_shapes=[
            pltpu.VMEM((seqs, span * heads, lanes), jnp.bfloat16),
            pltpu.VMEM((3, width, columns), jnp.bfloat16),
            pltpu.VMEM(out_weight.shape, jnp.bfloat16),
            pltpu.VMEM((seqs, 8, lanes), jnp.float32),
            pltpu.VMEM((seqs, span * heads), jnp.float32),
            pltpu.VMEM((seqs, 8, lanes), jnp.float32),
            pltpu.VMEM((seqs, heads, lanes), jnp.float32),
            pltpu.SemaphoreType.DMA((4,)),
            pltpu.SemaphoreType.DMA((seqs, parts)),
        ],
        compiler_params=pltpu.CompilerParams(vmem_limit_bytes=48 * 1024 * 1024),
    )(
        lengths,
        tokens,
        mixer_gain[None, :],
        jnp.tile(score_offset, lanes // heads)[None, :],
        jnp.broadcast_to(lengths[:, None], (seqs, lanes)),
        query_weight,
        key_weight,
        value_weight,
        out_weight,
        kv_cache.reshape(seqs, span * heads, lanes),
    )


def expert_apply(arrived_rows, gate_weight, up_weight, down_weight):
    gate_rows = jnp.dot(arrived_rows, gate_weight[0], preferred_element_type=jnp.float32)
    upward = jnp.dot(arrived_rows, up_weight[0], preferred_element_type=jnp.float32)
    active = (jax.nn.silu(gate_rows) * upward).astype(jnp.bfloat16)
    partial_rows = jnp.dot(active, down_weight[0], preferred_element_type=jnp.float32)
    return lax.psum_scatter(
        partial_rows.astype(jnp.bfloat16), "tp", scatter_dimension=1, tiled=True
    )


def per_device(
    tokens,
    kv_cache,
    lengths,
    score_offset,
    mixer_gain,
    query_weight,
    key_weight,
    value_weight,
    out_weight,
    channel_gain,
    routes,
    route_weights,
    gate_weight,
    up_weight,
    down_weight,
):
    seq_dev = tokens.shape[0]
    model_width = tokens.shape[1]
    experts = lax.axis_size("ep")
    top_count = routes.shape[1]
    capacity = max(2, 2 * seq_dev * top_count // experts)
    col_width = model_width // lax.axis_size("tp")
    col_start = lax.axis_index("tp") * col_width
    inputs = tokens.astype(jnp.float32)
    partial_out, new_entries = attend(
        tokens, kv_cache, lengths, score_offset, mixer_gain, query_weight, key_weight, value_weight, out_weight
    )
    mixed_heads = lax.psum(partial_out, "tp").astype(jnp.float32)
    residual = inputs + mixed_heads
    hidden = rms_scale(residual, channel_gain).astype(jnp.bfloat16)
    residual_cols = lax.dynamic_slice_in_dim(residual, col_start, col_width, 1)
    flat_routes = routes.reshape(-1)
    pair_count = flat_routes.shape[0]
    pair_index = jnp.arange(pair_count, dtype=jnp.int32)
    earlier = (flat_routes[None, :] == flat_routes[:, None]) & (
        pair_index[None, :] < pair_index[:, None]
    )
    slot_rank = jnp.sum(earlier.astype(jnp.int32), axis=1)
    slot_index = flat_routes * capacity + slot_rank
    slot_table = (
        slot_index[:, None] == jnp.arange(experts * capacity, dtype=jnp.int32)[None, :]
    ).astype(jnp.bfloat16)
    token_table = (
        (pair_index // top_count)[:, None] == jnp.arange(seq_dev, dtype=jnp.int32)[None, :]
    ).astype(jnp.bfloat16)
    placing = lax.dot_general(
        slot_table, token_table, (((0,), (0,)), ((), ())), preferred_element_type=jnp.float32
    ).astype(jnp.bfloat16)
    outgoing = (
        jnp.dot(placing, hidden, preferred_element_type=jnp.float32)
        .astype(jnp.bfloat16)
        .reshape(experts, capacity, model_width)
    )
    arrived = lax.all_to_all(outgoing, "ep", split_axis=0, concat_axis=0, tiled=True)
    sources = arrived.shape[0]
    item_count = arrived.shape[1]
    served = expert_apply(
        arrived.reshape(sources * item_count, model_width), gate_weight, up_weight, down_weight
    )
    returned = lax.all_to_all(
        served.reshape(sources, item_count, col_width),
        "ep",
        split_axis=0,
        concat_axis=0,
        tiled=True,
    )
    picked = (
        jnp.take(returned.reshape(experts * capacity, col_width), slot_index, axis=0)
        .astype(jnp.float32)
        .reshape(seq_dev, top_count, col_width)
    )
    expert_mix = jnp.sum(route_weights[:, :, None] * picked, axis=1)
    mixed = (residual_cols + expert_mix).astype(jnp.bfloat16)
    return (mixed, new_entries)


def solution(mesh):
    placed = (
        P("ep", None),
        P("ep", None, "tp", None),
        P("ep"),
        P("tp"),
        P(),
        P(None, "tp"),
        P(None, "tp"),
        P(None, "tp"),
        P("tp", None),
        P(),
        P("ep", None),
        P("ep", None),
        P("ep", None, "tp"),
        P("ep", None, "tp"),
        P("ep", "tp", None),
    )
    return jax.shard_map(
        per_device,
        mesh=mesh,
        in_specs=placed,
        out_specs=(P("ep", "tp"), P("ep", "tp", None)),
        check_vma=False,
    )
```

```python
import jax
import jax.numpy as jnp
from jax import lax
from jax.experimental import pallas as pl
from jax.experimental.pallas import tpu as pltpu
from jax.sharding import PartitionSpec as P

EPSILON = 1e-06
MESH = pl.DeviceIdType.MESH


def rms_scale(values, scale_gain):
    return (
        values * lax.rsqrt(jnp.mean(values * values, axis=-1, keepdims=True) + EPSILON) * scale_gain
    )


def attend_kernel(
    lengths_ref,
    tokens_ref,
    gain_ref,
    offset_ref,
    length_rows_ref,
    query_hbm,
    key_hbm,
    value_hbm,
    out_hbm,
    cache_hbm,
    partial_ref,
    entries_ref,
    cache_buf,
    weight_buf,
    out_buf,
    query_scr,
    score_scr,
    sum_scr,
    entry_scr,
    weight_sem,
    cache_sem,
):
    seqs, rows_all, lanes = cache_buf.shape
    heads = entries_ref.shape[1]
    head_dim = lanes // 2
    parts = cache_sem.shape[1]
    part_rows = rows_all // parts
    part_span = part_rows // heads
    blocks = rows_all // lanes
    block_span = lanes // heads

    def weight_copy(source, target, index):
        return pltpu.make_async_copy(source, target, weight_sem.at[index])

    copies = [
        weight_copy(query_hbm, weight_buf.at[0], 0),
        weight_copy(key_hbm, weight_buf.at[1], 1),
        weight_copy(value_hbm, weight_buf.at[2], 2),
        weight_copy(out_hbm, out_buf, 3),
    ]
    copies[0].start()

    def cache_copy(seq, part):
        span = pl.ds(part * part_rows, part_rows)
        return pltpu.make_async_copy(
            cache_hbm.at[seq, span], cache_buf.at[seq, span], cache_sem.at[seq, part]
        )

    def start_seq(seq, carry):
        for part in range(parts):

            @pl.when(lengths_ref[seq] > part * part_span)
            def _():
                cache_copy(seq, part).start()

        return carry

    lax.fori_loop(0, 2, start_seq, 0)
    copies[1].start()
    copies[2].start()
    lax.fori_loop(2, seqs, start_seq, 0)
    copies[3].start()

    inputs = tokens_ref[...].astype(jnp.float32)
    normed = rms_scale(inputs, gain_ref[...]).astype(jnp.bfloat16)
    query_scr[...] = jnp.zeros_like(query_scr)
    sum_scr[...] = jnp.zeros_like(sum_scr)
    copies[0].wait()
    query = jnp.dot(normed, weight_buf[0], preferred_element_type=jnp.float32)
    for head in range(heads):
        query_scr[:, head, :head_dim] = query[:, head * head_dim : (head + 1) * head_dim]

    group = query_scr.shape[1]
    row_id = lax.broadcasted_iota(jnp.int32, (group, part_rows), 0)
    lane_id = lax.broadcasted_iota(jnp.int32, (group, part_rows), 1)
    own_head = row_id == lane_id % heads

    def score_seq(seq, carry):
        query_rows = query_scr[seq].astype(jnp.bfloat16)
        for part in range(parts):

            @pl.when(lengths_ref[seq] > part * part_span)
            def _():
                cache_copy(seq, part).wait()
                rows = cache_buf[seq, part * part_rows : (part + 1) * part_rows, :]
                every = lax.dot_general(
                    query_rows, rows, (((1,), (1,)), ((), ())), preferred_element_type=jnp.float32
                )
                score_scr[pl.ds(seq, 1), part * part_rows : (part + 1) * part_rows] = jnp.sum(
                    jnp.where(own_head, every, 0.0), axis=0, keepdims=True
                )

        return carry

    lax.fori_loop(0, seqs, score_seq, 0)

    length_rows = length_rows_ref[...]
    offsets = offset_ref[...]
    lane = lax.broadcasted_iota(jnp.int32, (seqs, lanes), 1) // heads
    scores, keeps = [], []
    for block in range(blocks):
        visible = lane + block * block_span < length_rows
        score = score_scr[:, block * lanes : (block + 1) * lanes] * head_dim ** (-0.5) - offsets
        score = jnp.where(visible, score, 0.0)
        keep = -(jnp.maximum(score, 0.0) + jnp.log(1.0 + jnp.exp(-jnp.abs(score))))
        keep = jnp.where(visible, keep, 0.0)
        score_scr[:, block * lanes : (block + 1) * lanes] = score + keep
        keeps.append(keep)
    keep_all = jnp.concatenate(keeps, axis=0)
    keep_high = keep_all.astype(jnp.bfloat16)
    keep_low = (keep_all - keep_high.astype(jnp.float32)).astype(jnp.bfloat16)
    from_id = lax.broadcasted_iota(jnp.int32, (2 * lanes, 2 * lanes), 0) % lanes
    to_id = lax.broadcasted_iota(jnp.int32, (2 * lanes, 2 * lanes), 1)
    same = from_id % heads == to_id % heads
    later = (to_id >= lanes) | (from_id // heads > (to_id % lanes) // heads)
    summing = jnp.where(same & later, 1.0, 0.0).astype(jnp.bfloat16)
    summed = jnp.dot(
        jnp.concatenate([keep_high, keep_low], axis=1), summing, preferred_element_type=jnp.float32
    )
    carry = jnp.zeros((seqs, lanes), jnp.float32)
    for block in reversed(range(blocks)):
        visible = lane + block * block_span < length_rows
        piece = summed[block * seqs : (block + 1) * seqs]
        exponent = score_scr[:, block * lanes : (block + 1) * lanes] + piece[:, :lanes] + carry
        score_scr[:, block * lanes : (block + 1) * lanes] = jnp.where(
            visible, jnp.exp(exponent), 0.0
        )
        carry = carry + piece[:, lanes:]

    def value_seq(seq, carry):
        for part in range(parts):

            @pl.when(lengths_ref[seq] > part * part_span)
            def _():
                rows = cache_buf[seq, part * part_rows : (part + 1) * part_rows, :]
                sticks = score_scr[pl.ds(seq, 1), part * part_rows : (part + 1) * part_rows]
                sticks = jnp.where(
                    own_head, jnp.broadcast_to(sticks, own_head.shape), 0.0
                ).astype(jnp.bfloat16)
                sum_scr[seq] += jnp.dot(sticks, rows, preferred_element_type=jnp.float32)

        return carry

    lax.fori_loop(0, seqs, value_seq, 0)

    copies[1].wait()
    copies[2].wait()
    key = jnp.dot(normed, weight_buf[1], preferred_element_type=jnp.float32)
    value = jnp.dot(normed, weight_buf[2], preferred_element_type=jnp.float32)
    for head in range(heads):
        span = slice(head * head_dim, (head + 1) * head_dim)
        entry_scr[:, head, :] = jnp.concatenate([key[:, span], value[:, span]], axis=1)
    entries_ref[...] = entry_scr[...].astype(entries_ref.dtype)

    attended = jnp.concatenate(
        [sum_scr[:, head, head_dim:] for head in range(heads)], axis=1
    ).astype(jnp.bfloat16)
    copies[3].wait()
    partial_ref[...] = jnp.dot(
        attended, out_buf[...], preferred_element_type=jnp.float32
    ).astype(partial_ref.dtype)


def attend(
    tokens, kv_cache, lengths, score_offset, mixer_gain, query_weight, key_weight, value_weight, out_weight
):
    seqs, span, heads, lanes = kv_cache.shape
    width = tokens.shape[1]
    columns = query_weight.shape[1]
    parts = 4 if span % 4 == 0 and (span // 4 * heads) % lanes == 0 else 1
    vmem = pl.BlockSpec(memory_space=pltpu.VMEM)
    hbm = pl.BlockSpec(memory_space=pltpu.HBM)
    return pl.pallas_call(
        attend_kernel,
        name="attend",
        out_shape=(
            jax.ShapeDtypeStruct((seqs, width), jnp.bfloat16),
            jax.ShapeDtypeStruct((seqs, heads, lanes), jnp.bfloat16),
        ),
        in_specs=[pl.BlockSpec(memory_space=pltpu.SMEM)] + [vmem] * 4 + [hbm] * 5,
        out_specs=(vmem, vmem),
        scratch_shapes=[
            pltpu.VMEM((seqs, span * heads, lanes), jnp.bfloat16),
            pltpu.VMEM((3, width, columns), jnp.bfloat16),
            pltpu.VMEM(out_weight.shape, jnp.bfloat16),
            pltpu.VMEM((seqs, 8, lanes), jnp.float32),
            pltpu.VMEM((seqs, span * heads), jnp.float32),
            pltpu.VMEM((seqs, 8, lanes), jnp.float32),
            pltpu.VMEM((seqs, heads, lanes), jnp.float32),
            pltpu.SemaphoreType.DMA((4,)),
            pltpu.SemaphoreType.DMA((seqs, parts)),
        ],
        compiler_params=pltpu.CompilerParams(vmem_limit_bytes=48 * 1024 * 1024),
    )(
        lengths,
        tokens,
        mixer_gain[None, :],
        jnp.tile(score_offset, lanes // heads)[None, :],
        jnp.broadcast_to(lengths[:, None], (seqs, lanes)),
        query_weight,
        key_weight,
        value_weight,
        out_weight,
        kv_cache.reshape(seqs, span * heads, lanes),
    )


def mix_kernel(
    tokens_ref,
    partial_ref,
    gain_ref,
    routes_ref,
    route_weights_ref,
    gate_hbm,
    up_hbm,
    down_hbm,
    mixed_ref,
    gate_buf,
    up_buf,
    down_buf,
    head_slots,
    row_out,
    row_in,
    term_out,
    term_in,
    weight_sem,
    head_send,
    head_recv,
    row_send,
    row_recv,
    term_send,
    term_recv,
):
    experts, ranks, capacity, col_width = term_out.shape
    slots = experts * capacity
    seqs, width = tokens_ref.shape
    top_count = routes_ref.shape[1]
    my_ep = lax.axis_index("ep")
    my_tp = lax.axis_index("tp")
    me = my_ep * ranks + my_tp
    devices = experts * ranks

    def device(ep, tp):
        return {"ep": ep, "tp": tp}

    barrier = pltpu.get_barrier_semaphore()

    def greet(step, carry):
        peer = lax.rem(me + step, devices)
        pl.semaphore_signal(
            barrier, inc=1, device_id=device(peer // ranks, peer % ranks), device_id_type=MESH
        )
        return carry

    lax.fori_loop(1, devices, greet, 0)
    copies = [
        pltpu.make_async_copy(source.at[0], target, weight_sem.at[index])
        for index, (source, target) in enumerate(
            ((gate_hbm, gate_buf), (up_hbm, up_buf), (down_hbm, down_buf))
        )
    ]
    for copy in copies:
        copy.start()

    expert_id = lax.broadcasted_iota(jnp.int32, (seqs, experts), 1)
    earlier = (
        lax.broadcasted_iota(jnp.int32, (seqs, seqs), 0)
        > lax.broadcasted_iota(jnp.int32, (seqs, seqs), 1)
    ).astype(jnp.float32)
    slot_id = lax.broadcasted_iota(jnp.int32, (seqs, slots), 1)
    before = jnp.zeros((1, experts), jnp.float32)
    tables = []
    for choice in range(top_count):
        named = (routes_ref[:, choice : choice + 1] == expert_id).astype(jnp.float32)
        rank = jnp.dot(earlier, named, preferred_element_type=jnp.float32) + before
        slot = jnp.sum(
            named * (rank + (expert_id * capacity).astype(jnp.float32)), axis=1, keepdims=True
        )
        tables.append((slot.astype(jnp.int32) == slot_id).astype(jnp.float32))
        before = before + jnp.sum(named, axis=0, keepdims=True)
    placing = sum(tables).T.astype(jnp.bfloat16)

    pl.semaphore_wait(barrier, devices - 1)

    def head_copy(peer, slot):
        return pltpu.make_async_remote_copy(
            src_ref=partial_ref,
            dst_ref=head_slots.at[slot],
            send_sem=head_send.at[peer],
            recv_sem=head_recv.at[slot],
            device_id=device(my_ep, peer),
            device_id_type=MESH,
        )

    def row_copy(peer, slot):
        return pltpu.make_async_remote_copy(
            src_ref=row_out.at[peer],
            dst_ref=row_in.at[slot],
            send_sem=row_send.at[peer],
            recv_sem=row_recv.at[slot],
            device_id=device(peer, my_tp),
            device_id_type=MESH,
        )

    def term_copy(ep, tp, slot_ep, slot_tp):
        return pltpu.make_async_remote_copy(
            src_ref=term_out.at[ep, tp],
            dst_ref=term_in.at[slot_ep, slot_tp],
            send_sem=term_send.at[ep, tp],
            recv_sem=term_recv.at[slot_ep, slot_tp],
            device_id=device(ep, tp),
            device_id_type=MESH,
        )

    tp_peers = [lax.rem(my_tp + step, ranks) for step in range(1, ranks)]
    ep_peers = [lax.rem(my_ep + step, experts) for step in range(1, experts)]

    for peer in tp_peers:
        head_copy(peer, my_tp).start()
    head_slots[my_tp] = partial_ref[...]
    for peer in tp_peers:
        head_copy(peer, peer).wait_recv()
    heads_sum = head_slots[0].astype(jnp.float32)
    for rank in range(1, ranks):
        heads_sum = heads_sum + head_slots[rank].astype(jnp.float32)
    residual = tokens_ref[...].astype(jnp.float32) + heads_sum
    hidden = rms_scale(residual, gain_ref[...]).astype(jnp.bfloat16)
    rows = jnp.dot(placing, hidden, preferred_element_type=jnp.float32)
    row_out[...] = rows.reshape(experts, capacity, width).astype(jnp.bfloat16)
    for peer in ep_peers:
        row_copy(peer, my_ep).start()
    row_in[my_ep] = row_out[my_ep]
    residual_cols = jnp.zeros((seqs, col_width), jnp.float32)
    for rank in range(ranks):
        residual_cols = jnp.where(
            my_tp == rank, residual[:, rank * col_width : (rank + 1) * col_width], residual_cols
        )
    copies[0].wait()
    copies[1].wait()
    copies[2].wait()
    for peer in ep_peers:
        row_copy(peer, peer).wait_recv()

    arrived = row_in[...].astype(jnp.float32).reshape(slots, width).astype(jnp.bfloat16)
    gate_rows = jnp.dot(arrived, gate_buf[...], preferred_element_type=jnp.float32)
    upward = jnp.dot(arrived, up_buf[...], preferred_element_type=jnp.float32)
    active = (gate_rows / (1.0 + jnp.exp(-gate_rows)) * upward).astype(jnp.bfloat16)
    terms = jnp.dot(active, down_buf[...], preferred_element_type=jnp.float32)
    for rank in range(ranks):
        term_out[:, rank] = (
            terms[:, rank * col_width : (rank + 1) * col_width]
            .reshape(experts, capacity, col_width)
            .astype(jnp.bfloat16)
        )

    def send_term(step, carry):
        peer = lax.rem(me + step, devices)
        term_copy(peer // ranks, peer % ranks, my_ep, my_tp).start()
        return carry

    def take_term(step, carry):
        peer = lax.rem(me + step, devices)
        term_copy(peer // ranks, peer % ranks, peer // ranks, peer % ranks).wait_recv()
        return carry

    def sent_term(step, carry):
        peer = lax.rem(me + step, devices)
        term_copy(peer // ranks, peer % ranks, my_ep, my_tp).wait_send()
        return carry

    lax.fori_loop(1, devices, send_term, 0)
    term_in[my_ep, my_tp] = term_out[my_ep, my_tp]
    for peer in tp_peers:
        head_copy(peer, my_tp).wait_send()
    for peer in ep_peers:
        row_copy(peer, my_ep).wait_send()
    lax.fori_loop(1, devices, take_term, 0)
    returned = term_in[:, 0].astype(jnp.float32)
    for rank in range(1, ranks):
        returned = returned + term_in[:, rank].astype(jnp.float32)
    returned = returned.reshape(slots, col_width).astype(jnp.bfloat16)
    expert_mix = jnp.zeros((seqs, col_width), jnp.float32)
    for choice in range(top_count):
        picked = jnp.dot(
            tables[choice].astype(jnp.bfloat16), returned, preferred_element_type=jnp.float32
        )
        expert_mix = expert_mix + route_weights_ref[:, choice : choice + 1] * picked
    mixed_ref[...] = (residual_cols + expert_mix).astype(mixed_ref.dtype)
    lax.fori_loop(1, devices, sent_term, 0)


def mix(tokens, partial_out, channel_gain, routes, route_weights, gate_weight, up_weight, down_weight):
    seqs, width = tokens.shape
    experts = lax.axis_size("ep")
    ranks = lax.axis_size("tp")
    col_width = width // ranks
    needed = min(seqs, max(2, 2 * seqs * routes.shape[1] // experts))
    capacity = -(-needed // 8) * 8
    vmem = pl.BlockSpec(memory_space=pltpu.VMEM)
    hbm = pl.BlockSpec(memory_space=pltpu.HBM)
    dma = pltpu.SemaphoreType.DMA
    return pl.pallas_call(
        mix_kernel,
        name="mix",
        out_shape=jax.ShapeDtypeStruct((seqs, col_width), jnp.bfloat16),
        in_specs=[vmem] * 5 + [hbm] * 3,
        out_specs=vmem,
        scratch_shapes=[
            pltpu.VMEM(gate_weight.shape[1:], jnp.bfloat16),
            pltpu.VMEM(up_weight.shape[1:], jnp.bfloat16),
            pltpu.VMEM(down_weight.shape[1:], jnp.bfloat16),
            pltpu.VMEM((ranks, seqs, width), jnp.bfloat16),
            pltpu.VMEM((experts, capacity, width), jnp.bfloat16),
            pltpu.VMEM((experts, capacity, width), jnp.bfloat16),
            pltpu.VMEM((experts, ranks, capacity, col_width), jnp.bfloat16),
            pltpu.VMEM((experts, ranks, capacity, col_width), jnp.bfloat16),
            dma((3,)),
            dma((ranks,)),
            dma((ranks,)),
            dma((experts,)),
            dma((experts,)),
            dma((experts, ranks)),
            dma((experts, ranks)),
        ],
        compiler_params=pltpu.CompilerParams(
            collective_id=1, has_side_effects=True, vmem_limit_bytes=32 * 1024 * 1024
        ),
    )(
        tokens,
        partial_out,
        channel_gain[None, :],
        routes,
        route_weights,
        gate_weight,
        up_weight,
        down_weight,
    )


def per_device(
    tokens,
    kv_cache,
    lengths,
    score_offset,
    mixer_gain,
    query_weight,
    key_weight,
    value_weight,
    out_weight,
    channel_gain,
    routes,
    route_weights,
    gate_weight,
    up_weight,
    down_weight,
):
    partial_out, new_entries = attend(
        tokens, kv_cache, lengths, score_offset, mixer_gain, query_weight, key_weight, value_weight, out_weight
    )
    mixed = mix(
        tokens, partial_out, channel_gain, routes, route_weights, gate_weight, up_weight, down_weight
    )
    return (mixed, new_entries)


def solution(mesh):
    placed = (
        P("ep", None),
        P("ep", None, "tp", None),
        P("ep"),
        P("tp"),
        P(),
        P(None, "tp"),
        P(None, "tp"),
        P(None, "tp"),
        P("tp", None),
        P(),
        P("ep", None),
        P("ep", None),
        P("ep", None, "tp"),
        P("ep", None, "tp"),
        P("ep", "tp", None),
    )
    return jax.shard_map(
        per_device,
        mesh=mesh,
        in_specs=placed,
        out_specs=(P("ep", "tp"), P("ep", "tp", None)),
        check_vma=False,
    )
```

```python
import jax
import jax.numpy as jnp
from jax import lax
from jax.experimental import pallas as pl
from jax.experimental.pallas import tpu as pltpu
from jax.sharding import PartitionSpec as P

EPSILON = 1e-06
MESH = pl.DeviceIdType.MESH
VMEM_LIMIT = 67043328


def rms_scale(values, scale_gain):
    return (
        values * lax.rsqrt(jnp.mean(values * values, axis=-1, keepdims=True) + EPSILON) * scale_gain
    )


def attend_kernel(
    lengths_ref,
    offset_ref,
    tokens_hbm,
    gain_hbm,
    query_hbm,
    key_hbm,
    value_hbm,
    out_hbm,
    cache_hbm,
    partial_ref,
    entries_ref,
    cache_buf,
    tokens_buf,
    gain_buf,
    weight_buf,
    out_buf,
    query_scr,
    score_scr,
    sum_scr,
    entry_scr,
    weight_sem,
    cache_sem,
):
    seqs, rows_all, lanes = cache_buf.shape
    heads = entries_ref.shape[1]
    head_dim = lanes // 2
    parts = cache_sem.shape[1]
    part_rows = rows_all // parts
    part_span = part_rows // heads
    blocks = rows_all // lanes
    block_span = lanes // heads

    def weight_copy(source, target, index):
        return pltpu.make_async_copy(source, target, weight_sem.at[index])

    copies = [
        weight_copy(query_hbm, weight_buf.at[0], 0),
        weight_copy(key_hbm, weight_buf.at[1], 1),
        weight_copy(value_hbm, weight_buf.at[2], 2),
        weight_copy(out_hbm, out_buf, 3),
        weight_copy(tokens_hbm, tokens_buf, 4),
        weight_copy(gain_hbm, gain_buf, 5),
    ]
    copies[4].start()
    copies[5].start()
    copies[0].start()

    def cache_copy(seq, part):
        span = pl.ds(part * part_rows, part_rows)
        return pltpu.make_async_copy(
            cache_hbm.at[seq, span], cache_buf.at[seq, span], cache_sem.at[seq, part]
        )

    def start_seq(seq, carry):
        for part in range(parts):

            needed = lengths_ref[seq] > part * part_span

            @pl.when(needed)
            def _():
                cache_copy(seq, part).start()

            @pl.when(jnp.logical_not(needed))
            def _():
                cache_buf[seq, part * part_rows : (part + 1) * part_rows, :] = jnp.zeros(
                    (part_rows, lanes), cache_buf.dtype
                )

        return carry

    lax.fori_loop(0, 2, start_seq, 0)
    copies[1].start()
    copies[2].start()
    lax.fori_loop(2, seqs, start_seq, 0)
    copies[3].start()

    copies[4].wait()
    copies[5].wait()
    inputs = tokens_buf[...].astype(jnp.float32)
    normed = rms_scale(inputs, gain_buf[...]).astype(jnp.bfloat16)
    query_scr[...] = jnp.zeros_like(query_scr)
    copies[0].wait()
    query = jnp.dot(normed, weight_buf[0], preferred_element_type=jnp.float32)
    for head in range(heads):
        query_scr[:, head, :head_dim] = query[:, head * head_dim : (head + 1) * head_dim]

    copies[1].wait()
    copies[2].wait()
    key = jnp.dot(normed, weight_buf[1], preferred_element_type=jnp.float32)
    value = jnp.dot(normed, weight_buf[2], preferred_element_type=jnp.float32)
    for head in range(heads):
        span = slice(head * head_dim, (head + 1) * head_dim)
        entry_scr[:, head, :] = jnp.concatenate([key[:, span], value[:, span]], axis=1)
    entries_ref[...] = entry_scr[...].astype(entries_ref.dtype)

    group = query_scr.shape[1]
    row_id = lax.broadcasted_iota(jnp.int32, (group, rows_all), 0)
    lane_id = lax.broadcasted_iota(jnp.int32, (group, rows_all), 1)
    own_head = row_id == lane_id % heads
    together = 2 if seqs % 2 == 0 else 1

    def score_seqs(step, carry):
        first = step * together
        for member in range(together):
            for part in range(parts):

                @pl.when(lengths_ref[first + member] > part * part_span)
                def _():
                    cache_copy(first + member, part).wait()

        for member in range(together):
            seq = first + member
            every = lax.dot_general(
                query_scr[seq].astype(jnp.bfloat16),
                cache_buf[seq],
                (((1,), (1,)), ((), ())),
                preferred_element_type=jnp.float32,
            )
            score_scr[pl.ds(seq, 1), :] = jnp.sum(
                jnp.where(own_head, every, 0.0), axis=0, keepdims=True
            )
        return carry

    lax.fori_loop(0, seqs // together, score_seqs, 0)

    seq_id = lax.broadcasted_iota(jnp.int32, (seqs, lanes), 0)
    length_rows = jnp.zeros((seqs, lanes), jnp.int32)
    for seq in range(seqs):
        length_rows = jnp.where(seq_id == seq, lengths_ref[seq], length_rows)
    head_id = lax.broadcasted_iota(jnp.int32, (seqs, lanes), 1) % heads
    offsets = jnp.zeros((seqs, lanes), jnp.float32)
    for head in range(heads):
        offsets = jnp.where(head_id == head, offset_ref[head], offsets)
    lane = lax.broadcasted_iota(jnp.int32, (seqs, lanes), 1) // heads
    scores, keeps = [], []
    for block in range(blocks):
        visible = lane + block * block_span < length_rows
        score = score_scr[:, block * lanes : (block + 1) * lanes] * head_dim ** (-0.5) - offsets
        score = jnp.where(visible, score, 0.0)
        keep = -(jnp.maximum(score, 0.0) + jnp.log(1.0 + jnp.exp(-jnp.abs(score))))
        keep = jnp.where(visible, keep, 0.0)
        score_scr[:, block * lanes : (block + 1) * lanes] = score + keep
        keeps.append(keep)
    keep_all = jnp.concatenate(keeps, axis=0)
    keep_high = keep_all.astype(jnp.bfloat16)
    keep_low = (keep_all - keep_high.astype(jnp.float32)).astype(jnp.bfloat16)
    from_id = lax.broadcasted_iota(jnp.int32, (2 * lanes, 2 * lanes), 0) % lanes
    to_id = lax.broadcasted_iota(jnp.int32, (2 * lanes, 2 * lanes), 1)
    same = from_id % heads == to_id % heads
    later = (to_id >= lanes) | (from_id // heads > (to_id % lanes) // heads)
    summing = jnp.where(same & later, 1.0, 0.0).astype(jnp.bfloat16)
    summed = jnp.dot(
        jnp.concatenate([keep_high, keep_low], axis=1), summing, preferred_element_type=jnp.float32
    )
    carry = jnp.zeros((seqs, lanes), jnp.float32)
    for block in reversed(range(blocks)):
        visible = lane + block * block_span < length_rows
        piece = summed[block * seqs : (block + 1) * seqs]
        exponent = score_scr[:, block * lanes : (block + 1) * lanes] + piece[:, :lanes] + carry
        score_scr[:, block * lanes : (block + 1) * lanes] = jnp.where(
            visible, jnp.exp(exponent), 0.0
        )
        carry = carry + piece[:, lanes:]

    for seq in range(seqs):
        sticks = jnp.where(
            own_head, jnp.broadcast_to(score_scr[seq : seq + 1, :], own_head.shape), 0.0
        ).astype(jnp.bfloat16)
        sum_scr[seq] = jnp.dot(sticks, cache_buf[seq], preferred_element_type=jnp.float32)

    attended = jnp.concatenate(
        [sum_scr[:, head, head_dim:] for head in range(heads)], axis=1
    ).astype(jnp.bfloat16)
    copies[3].wait()
    partial_ref[...] = jnp.dot(
        attended, out_buf[...], preferred_element_type=jnp.float32
    ).astype(partial_ref.dtype)


def attend(
    tokens, kv_cache, lengths, score_offset, mixer_gain, query_weight, key_weight, value_weight, out_weight
):
    seqs, span, heads, lanes = kv_cache.shape
    width = tokens.shape[1]
    columns = query_weight.shape[1]
    parts = 4 if span % 4 == 0 and (span // 4 * heads) % lanes == 0 else 1
    vmem = pl.BlockSpec(memory_space=pltpu.VMEM)
    hbm = pl.BlockSpec(memory_space=pltpu.HBM)
    return pl.pallas_call(
        attend_kernel,
        name="attend",
        out_shape=(
            jax.ShapeDtypeStruct((seqs, width), jnp.bfloat16),
            jax.ShapeDtypeStruct((seqs, heads, lanes), jnp.bfloat16),
        ),
        in_specs=[pl.BlockSpec(memory_space=pltpu.SMEM)] * 2 + [hbm] * 7,
        out_specs=(vmem, vmem),
        scratch_shapes=[
            pltpu.VMEM((seqs, span * heads, lanes), jnp.bfloat16),
            pltpu.VMEM((seqs, width), jnp.bfloat16),
            pltpu.VMEM((1, width), jnp.float32),
            pltpu.VMEM((3, width, columns), jnp.bfloat16),
            pltpu.VMEM(out_weight.shape, jnp.bfloat16),
            pltpu.VMEM((seqs, 8, lanes), jnp.float32),
            pltpu.VMEM((seqs, span * heads), jnp.float32),
            pltpu.VMEM((seqs, 8, lanes), jnp.float32),
            pltpu.VMEM((seqs, heads, lanes), jnp.float32),
            pltpu.SemaphoreType.DMA((6,)),
            pltpu.SemaphoreType.DMA((seqs, parts)),
        ],
        compiler_params=pltpu.CompilerParams(vmem_limit_bytes=VMEM_LIMIT),
    )(
        lengths,
        score_offset,
        tokens,
        mixer_gain[None, :],
        query_weight,
        key_weight,
        value_weight,
        out_weight,
        kv_cache.reshape(seqs, span * heads, lanes),
    )


def mix_kernel(
    tokens_hbm,
    partial_hbm,
    gain_hbm,
    routes_hbm,
    route_weights_hbm,
    gate_hbm,
    up_hbm,
    down_hbm,
    mixed_ref,
    tokens_ref,
    gain_ref,
    routes_ref,
    route_weights_ref,
    gate_buf,
    up_buf,
    down_buf,
    head_slots,
    row_out,
    row_in,
    term_out,
    term_in,
    weight_sem,
    head_send,
    head_recv,
    row_send,
    row_recv,
    term_send,
    term_recv,
):
    experts, ranks, capacity, col_width = term_out.shape
    slots = experts * capacity
    seqs, width = tokens_ref.shape
    top_count = routes_ref.shape[0]
    my_ep = lax.axis_index("ep")
    my_tp = lax.axis_index("tp")
    me = my_ep * ranks + my_tp
    devices = experts * ranks

    def device(ep, tp):
        return {"ep": ep, "tp": tp}

    barrier = pltpu.get_barrier_semaphore()

    def greet(step, carry):
        peer = lax.rem(me + step, devices)
        pl.semaphore_signal(
            barrier, inc=1, device_id=device(peer // ranks, peer % ranks), device_id_type=MESH
        )
        return carry

    lax.fori_loop(1, devices, greet, 0)
    copies = [
        pltpu.make_async_copy(source, target, weight_sem.at[index])
        for index, (source, target) in enumerate(
            (
                (gate_hbm.at[0], gate_buf),
                (up_hbm.at[0], up_buf),
                (down_hbm.at[0], down_buf),
                (partial_hbm, head_slots.at[my_tp]),
                (routes_hbm, routes_ref),
                (route_weights_hbm, route_weights_ref),
                (tokens_hbm, tokens_ref),
                (gain_hbm, gain_ref),
            )
        )
    ]
    for index in (3, 4, 5, 6, 7, 0, 1, 2):
        copies[index].start()
    copies[4].wait()
    copies[5].wait()

    expert_id = lax.broadcasted_iota(jnp.int32, (seqs, experts), 1)
    earlier = (
        lax.broadcasted_iota(jnp.int32, (seqs, seqs), 0)
        > lax.broadcasted_iota(jnp.int32, (seqs, seqs), 1)
    ).astype(jnp.float32)
    diagonal = lax.broadcasted_iota(jnp.int32, (seqs, seqs), 0) == lax.broadcasted_iota(
        jnp.int32, (seqs, seqs), 1
    )
    slot_id = lax.broadcasted_iota(jnp.int32, (seqs, slots), 1)

    def column(ref, choice):
        row = jnp.broadcast_to(ref[choice : choice + 1, :], (seqs, seqs)).astype(jnp.float32)
        return jnp.sum(jnp.where(diagonal, row, 0.0), axis=1, keepdims=True)

    before = jnp.zeros((1, experts), jnp.float32)
    tables = []
    for choice in range(top_count):
        named = (column(routes_ref, choice).astype(jnp.int32) == expert_id).astype(jnp.float32)
        rank = jnp.dot(earlier, named, preferred_element_type=jnp.float32) + before
        slot = jnp.sum(
            named * (rank + (expert_id * capacity).astype(jnp.float32)), axis=1, keepdims=True
        )
        tables.append((slot.astype(jnp.int32) == slot_id).astype(jnp.float32))
        before = before + jnp.sum(named, axis=0, keepdims=True)
    placing = sum(tables).T.astype(jnp.bfloat16)
    shares = [column(route_weights_ref, choice) for choice in range(top_count)]

    copies[3].wait()
    copies[6].wait()
    copies[7].wait()
    pl.semaphore_wait(barrier, devices - 1)

    def head_copy(peer, slot):
        return pltpu.make_async_remote_copy(
            src_ref=head_slots.at[my_tp],
            dst_ref=head_slots.at[slot],
            send_sem=head_send.at[peer],
            recv_sem=head_recv.at[slot],
            device_id=device(my_ep, peer),
            device_id_type=MESH,
        )

    def row_copy(peer, slot):
        return pltpu.make_async_remote_copy(
            src_ref=row_out.at[peer],
            dst_ref=row_in.at[slot],
            send_sem=row_send.at[peer],
            recv_sem=row_recv.at[slot],
            device_id=device(peer, my_tp),
            device_id_type=MESH,
        )

    def term_copy(ep, tp, slot_ep, slot_tp):
        return pltpu.make_async_remote_copy(
            src_ref=term_out.at[ep, tp],
            dst_ref=term_in.at[slot_ep, slot_tp],
            send_sem=term_send.at[ep, tp],
            recv_sem=term_recv.at[slot_ep, slot_tp],
            device_id=device(ep, tp),
            device_id_type=MESH,
        )

    tp_peers = [lax.rem(my_tp + step, ranks) for step in range(1, ranks)]
    far_first = sorted(range(1, experts), key=lambda step: -min(step, experts - step))
    ep_peers = [lax.rem(my_ep + step, experts) for step in far_first]

    for peer in tp_peers:
        head_copy(peer, my_tp).start()
    for peer in tp_peers:
        head_copy(peer, peer).wait_recv()
    heads_sum = head_slots[0].astype(jnp.float32)
    for rank in range(1, ranks):
        heads_sum = heads_sum + head_slots[rank].astype(jnp.float32)
    residual = tokens_ref[...].astype(jnp.float32) + heads_sum
    hidden = rms_scale(residual, gain_ref[...]).astype(jnp.bfloat16)
    rows = jnp.dot(placing, hidden, preferred_element_type=jnp.float32)
    row_out[...] = rows.reshape(experts, capacity, width).astype(jnp.bfloat16)
    for peer in ep_peers:
        row_copy(peer, my_ep).start()
    row_in[my_ep] = row_out[my_ep]
    residual_cols = jnp.zeros((seqs, col_width), jnp.float32)
    for rank in range(ranks):
        residual_cols = jnp.where(
            my_tp == rank, residual[:, rank * col_width : (rank + 1) * col_width], residual_cols
        )
    copies[0].wait()
    copies[1].wait()
    copies[2].wait()
    for peer in ep_peers:
        row_copy(peer, peer).wait_recv()

    arrived = row_in[...].astype(jnp.float32).reshape(slots, width).astype(jnp.bfloat16)
    gate_rows = jnp.dot(arrived, gate_buf[...], preferred_element_type=jnp.float32)
    upward = jnp.dot(arrived, up_buf[...], preferred_element_type=jnp.float32)
    active = (gate_rows / (1.0 + jnp.exp(-gate_rows)) * upward).astype(jnp.bfloat16)
    terms = jnp.dot(active, down_buf[...], preferred_element_type=jnp.float32)
    for rank in range(ranks):
        term_out[:, rank] = (
            terms[:, rank * col_width : (rank + 1) * col_width]
            .reshape(experts, capacity, col_width)
            .astype(jnp.bfloat16)
        )

    def send_term(step, carry):
        peer = lax.rem(me + 1 + lax.rem(step + devices * 3 // 8, devices - 1), devices)
        term_copy(peer // ranks, peer % ranks, my_ep, my_tp).start()
        return carry

    def take_term(step, carry):
        peer = lax.rem(me + step, devices)
        term_copy(peer // ranks, peer % ranks, peer // ranks, peer % ranks).wait_recv()
        return carry

    def sent_term(step, carry):
        peer = lax.rem(me + step, devices)
        term_copy(peer // ranks, peer % ranks, my_ep, my_tp).wait_send()
        return carry

    lax.fori_loop(1, devices, send_term, 0)
    term_in[my_ep, my_tp] = term_out[my_ep, my_tp]
    for peer in tp_peers:
        head_copy(peer, my_tp).wait_send()
    for peer in ep_peers:
        row_copy(peer, my_ep).wait_send()
    lax.fori_loop(1, devices, take_term, 0)
    returned = term_in[:, 0].astype(jnp.float32)
    for rank in range(1, ranks):
        returned = returned + term_in[:, rank].astype(jnp.float32)
    returned = returned.reshape(slots, col_width).astype(jnp.bfloat16)
    expert_mix = jnp.zeros((seqs, col_width), jnp.float32)
    for choice in range(top_count):
        picked = jnp.dot(
            tables[choice].astype(jnp.bfloat16), returned, preferred_element_type=jnp.float32
        )
        expert_mix = expert_mix + shares[choice] * picked
    mixed_ref[...] = (residual_cols + expert_mix).astype(mixed_ref.dtype)
    lax.fori_loop(1, devices, sent_term, 0)


def mix(tokens, partial_out, channel_gain, routes, route_weights, gate_weight, up_weight, down_weight):
    seqs, width = tokens.shape
    experts = lax.axis_size("ep")
    ranks = lax.axis_size("tp")
    col_width = width // ranks
    needed = min(seqs, max(2, 2 * seqs * routes.shape[1] // experts))
    capacity = -(-needed // 8) * 8
    vmem = pl.BlockSpec(memory_space=pltpu.VMEM)
    hbm = pl.BlockSpec(memory_space=pltpu.HBM)
    dma = pltpu.SemaphoreType.DMA
    return pl.pallas_call(
        mix_kernel,
        name="mix",
        out_shape=jax.ShapeDtypeStruct((seqs, col_width), jnp.bfloat16),
        in_specs=[hbm] * 8,
        out_specs=vmem,
        scratch_shapes=[
            pltpu.VMEM((seqs, width), jnp.bfloat16),
            pltpu.VMEM((1, width), jnp.float32),
            pltpu.VMEM(routes.shape[::-1], routes.dtype),
            pltpu.VMEM(route_weights.shape[::-1], route_weights.dtype),
            pltpu.VMEM(gate_weight.shape[1:], jnp.bfloat16),
            pltpu.VMEM(up_weight.shape[1:], jnp.bfloat16),
            pltpu.VMEM(down_weight.shape[1:], jnp.bfloat16),
            pltpu.VMEM((ranks, seqs, width), jnp.bfloat16),
            pltpu.VMEM((experts, capacity, width), jnp.bfloat16),
            pltpu.VMEM((experts, capacity, width), jnp.bfloat16),
            pltpu.VMEM((experts, ranks, capacity, col_width), jnp.bfloat16),
            pltpu.VMEM((experts, ranks, capacity, col_width), jnp.bfloat16),
            dma((8,)),
            dma((ranks,)),
            dma((ranks,)),
            dma((experts,)),
            dma((experts,)),
            dma((experts, ranks)),
            dma((experts, ranks)),
        ],
        compiler_params=pltpu.CompilerParams(
            collective_id=1, has_side_effects=True, vmem_limit_bytes=VMEM_LIMIT
        ),
    )(
        tokens,
        partial_out,
        channel_gain[None, :],
        routes.T,
        route_weights.T,
        gate_weight,
        up_weight,
        down_weight,
    )


def per_device(
    tokens,
    kv_cache,
    lengths,
    score_offset,
    mixer_gain,
    query_weight,
    key_weight,
    value_weight,
    out_weight,
    channel_gain,
    routes,
    route_weights,
    gate_weight,
    up_weight,
    down_weight,
):
    partial_out, new_entries = attend(
        tokens, kv_cache, lengths, score_offset, mixer_gain, query_weight, key_weight, value_weight, out_weight
    )
    mixed = mix(
        tokens, partial_out, channel_gain, routes, route_weights, gate_weight, up_weight, down_weight
    )
    return (mixed, new_entries)


def solution(mesh):
    placed = (
        P("ep", None),
        P("ep", None, "tp", None),
        P("ep"),
        P("tp"),
        P(),
        P(None, "tp"),
        P(None, "tp"),
        P(None, "tp"),
        P("tp", None),
        P(),
        P("ep", None),
        P("ep", None),
        P("ep", None, "tp"),
        P("ep", None, "tp"),
        P("ep", "tp", None),
    )
    return jax.shard_map(
        per_device,
        mesh=mesh,
        in_specs=placed,
        out_specs=(P("ep", "tp"), P("ep", "tp", None)),
        check_vma=False,
    )
```
